32 devices in a mesh: grp: 2 (over x), fs: 4 (over y, core), tp: 4 (over z).
Axes of the slice: x: 2, y: 2, z: 4, core: 2. Of those that a mesh axis runs over, the one named last changes fastest.
Arguments:
- prompt_tokens: bfloat16 [4096, 2048], P(('grp', 'fs', 'tp')), parts along dimension 0, may hold values from -6 to 6
- up_weight: float32 [2048, 8192], P('fs', 'tp'), may hold values from -0.125 to 0.125
- down_weight: float32 [2048, 8192], P('fs', 'tp'), may hold values from -0.0625 to 0.0625
- pre_gain: float32 [2048], P('fs'), may hold values from 0.1 to 1.9
- post_gain: float32 [2048], replicated, may hold values from 0.1 to 1.9
Outputs:
- mixed: bfloat16 [4096, 2048], P(('grp', 'fs', 'tp')), parts along dimension 0
- sampler_up: bfloat16 [4096, 8192], P('grp', 'tp'), parts along dimension 0
- sampler_down: bfloat16 [4096, 8192], P('grp', 'tp'), parts along dimension 0
The draws below stay inside these ranges and needn't reach their ends.
There are 2 independent parts, one for each index of `grp`. The reference program is written for one: setup_inputs(seed, part) draws one part's arguments, and reference() takes and returns one part's arrays. A program takes and returns all parts, laid end to end along the dimension named above; an argument that names none is the same for every part. Nothing has to cross between parts.
All inputs are finite; a program needn't handle non-finite values.
Results may differ from the reference program's by a relative error of at most 0.015.
Values may be sent and summed in bfloat16 or wider, within the bound.
A program may use at most 128 MiB of HBM per device.

```python
import jax
import jax.numpy as jnp
from jax import lax

D = 2048
FF = 8192
TOK_DEV = 128
TOKENS = 2048
N_TP = 4


def shard_levels(stream_key, extent, split, low, top_value):
    loudness = 1.0
    for dim, blocks in split:
        heights = jax.random.uniform(jax.random.fold_in(jax.random.fold_in(stream_key, 6), dim), (blocks,), jnp.float32, low / len(split), top_value / len(split))
        loudness = loudness * jnp.repeat(jnp.exp(heights), extent[dim] // blocks).reshape((-1,) + (1,) * (len(extent) - 1 - dim))
    return loudness


def gaussian(key, shape, scale, reach, shards=(), dtype=jnp.bfloat16):
    values = jax.random.normal(key, shape, jnp.float32) * scale
    if len(shards) > 0:
        values = shard_levels(key, shape, shards, -0.22, 0.18) * values
    return jnp.clip(values, min=-reach, max=reach).astype(dtype)


def setup_inputs(seed: int = 0, part: int = 0) -> dict:
    arg_keys = jax.random.split(jax.random.key(seed), 6)
    part_splits = jax.random.split(jax.random.fold_in(arg_keys[5], part), 6)
    return {
        "prompt_tokens": gaussian(part_splits[0], (TOKENS, D), 1.0, 6.0, ((0, 16),)),
        "up_weight": gaussian(arg_keys[1], (D, FF), D ** -0.5, 0.125, ((0, 4), (1, 4)), jnp.float32),
        "down_weight": gaussian(arg_keys[2], (D, FF), FF ** -0.5, 0.0625, ((0, 4), (1, 4)), jnp.float32),
        "pre_gain": jnp.clip(1.0 + 0.18 * jax.random.normal(arg_keys[3], (D,), jnp.float32), 0.1, 1.9),
        "post_gain": jnp.clip(1.0 + 0.18 * jax.random.normal(arg_keys[4], (D,), jnp.float32), 0.1, 1.9),
    }


def reference(prompt_tokens, up_weight, down_weight, pre_gain, post_gain):
    sampler_up = (up_weight * pre_gain[:, None]).astype(jnp.bfloat16)
    sampler_down = down_weight.astype(jnp.bfloat16)
    width = prompt_tokens.shape[1]
    hidden_units = up_weight.shape[1]
    block_rows = TOK_DEV * N_TP
    blocks = prompt_tokens.reshape(TOKENS // block_rows, block_rows, width)
    down_split = sampler_down.astype(jnp.float32).reshape(width, N_TP, hidden_units // N_TP)

    def one_block(rows):
        values = rows.astype(jnp.float32)
        normed = (values * lax.rsqrt(lax.optimization_barrier(jnp.mean(values * values, axis=1, keepdims=True)) + 1e-06)).astype(jnp.bfloat16)
        lifted = jnp.dot(normed, sampler_up, preferred_element_type=jnp.float32)
        hidden = jnp.square(jax.nn.relu(lifted)).astype(jnp.bfloat16)
        hidden_split = hidden.astype(jnp.float32).reshape(block_rows, N_TP, hidden_units // N_TP)
        parts = jnp.einsum('rbk,dbk->brd', hidden_split, down_split).astype(jnp.bfloat16)
        summed = lax.optimization_barrier(jnp.sum(parts.astype(jnp.float32), axis=0))
        scaled = summed * lax.rsqrt(lax.optimization_barrier(jnp.mean(summed * summed, axis=1, keepdims=True)) + 1e-06)
        return (scaled * post_gain[None, :]).astype(jnp.bfloat16)
    mixed = lax.map(one_block, blocks).reshape(TOKENS, width)
    return (mixed, sampler_up, sampler_down)
```

```python
import functools

import jax
import jax.numpy as jnp
from jax import lax
from jax.experimental import pallas as pl
from jax.experimental.pallas import tpu as pltpu
from jax.sharding import PartitionSpec as P

MESH = pl.DeviceIdType.MESH
BF16 = jnp.bfloat16
F32 = jnp.float32


def layer_kernel(sizes, tok_ref, gain_ref, post_ref, up_hbm, down_hbm, mixed_ref, up_full, down_full,
                 stage, tok, hidden, rbuf, sbuf, total,
                 load_sem, tsend, trecv, ysend, yrecv, xsend, xrecv, csend, crecv, osend, orecv, rsend, rrecv):
    G, F, T, NC = sizes
    Y = F // 2
    g, fs, z = lax.axis_index("grp"), lax.axis_index("fs"), lax.axis_index("tp")
    y, c = fs // 2, fs % 2
    R, H = up_hbm.shape
    piece = R // G
    CR = piece // NC
    rows_t = tok_ref.shape[0]
    full = (up_full, down_full)
    hbm = (up_hbm, down_hbm)
    partner = y * 2 + (1 - c)
    not_first, not_last = z > 0, z < T - 1

    def loads(m, e):
        r = pl.ds(pl.multiple_of(((g + e) % G) * piece, piece), piece)
        return pltpu.make_async_copy(hbm[m].at[r], stage.at[m, r], load_sem.at[m, e])

    for m in range(2):
        for e in range(G):
            loads(m, e).start()

    barrier = pltpu.get_barrier_semaphore()
    for d in range(1, Y):
        pl.semaphore_signal(barrier, inc=1, device_id={"fs": ((y + d) % Y) * 2 + c}, device_id_type=MESH)
    for e in range(1, G):
        pl.semaphore_signal(barrier, inc=1, device_id={"grp": (g + e) % G}, device_id_type=MESH)
    pl.semaphore_signal(barrier, inc=1, device_id={"fs": partner}, device_id_type=MESH)

    @pl.when(not_first)
    def _():
        pl.semaphore_signal(barrier, inc=1, device_id={"tp": z - 1}, device_id_type=MESH)

    @pl.when(not_last)
    def _():
        pl.semaphore_signal(barrier, inc=1, device_id={"tp": z + 1}, device_id_type=MESH)

    values = tok_ref[...].astype(F32)
    scale = lax.rsqrt(jnp.mean(values * values, axis=1, keepdims=True) + 1e-06)
    tok[z] = (values * scale).astype(BF16)

    def convert(m, start, n):
        for i in range(0, n, CR):
            r = pl.ds(pl.multiple_of(start + i, CR), CR)
            v = stage[m, r, :]
            if m == 0:
                v = v * gain_ref[r, :]
            full[m][pl.ds(pl.multiple_of(fs * R + start + i, CR), CR), :] = v.astype(BF16)

    def remote(ref, rows, ss, rs, dev):
        return pltpu.make_async_remote_copy(ref.at[rows], ref.at[rows], ss, rs, device_id=dev, device_id_type=MESH)

    def chunk_rows(shard, e, q):
        return pl.ds(pl.multiple_of(shard * R + ((g + e) % G) * piece + q * CR, CR), CR)

    def y_copy(m, d, q):
        return remote(full[m], chunk_rows(fs, 0, q), ysend.at[m, d, q], yrecv.at[m, d, q],
                      {"fs": ((y + d) % Y) * 2 + c})

    def y_in(m, d, q):
        shard = ((y - d + Y) % Y) * 2 + c
        return remote(full[m], chunk_rows(shard, 0, q), ysend.at[m, d, q], yrecv.at[m, d, q], {"fs": partner})

    def x_copy(m, d, q, e):
        shard = ((y - d + Y) % Y) * 2 + c
        return remote(full[m], chunk_rows(shard, 0, q), xsend.at[m, d, q, e], xrecv.at[m, d, q, e],
                      {"grp": (g + e) % G})

    def x_in(m, d, q, e):
        shard = ((y - d + Y) % Y) * 2 + c
        return remote(full[m], chunk_rows(shard, G - e, q), xsend.at[m, d, q, e], xrecv.at[m, d, q, e],
                      {"grp": (g + e) % G})

    def c_copy(m, d, q, e):
        shard = ((y - d + Y) % Y) * 2 + c
        return remote(full[m], chunk_rows(shard, (G - e) % G, q), csend.at[m, d, q, e], crecv.at[m, d, q, e],
                      {"fs": partner})

    def c_in(m, d, q, e):
        shard = ((y - d + Y) % Y) * 2 + (1 - c)
        return remote(full[m], chunk_rows(shard, (G - e) % G, q), csend.at[m, d, q, e], crecv.at[m, d, q, e],
                      {"fs": partner})

    def own_copy(m, sign):
        shard = fs if sign else partner
        r = pl.ds(pl.multiple_of(shard * R, R), R)
        return remote(full[m], r, osend.at[m], orecv.at[m], {"fs": partner})

    pl.semaphore_wait(barrier, (Y - 1) + (G - 1) + 1 + not_first.astype(jnp.int32) + not_last.astype(jnp.int32))

    def tok_out(dirn, k):
        b = z - k if dirn == 0 else z + k
        dev = z + 1 if dirn == 0 else z - 1
        return pltpu.make_async_remote_copy(tok.at[b], tok.at[b], tsend.at[dirn, k], trecv.at[dirn, k],
                                            device_id={"tp": dev}, device_id_type=MESH)

    def tok_in(dirn, k):
        b = z - k - 1 if dirn == 0 else z + k + 1
        dev = z + 1 if dirn == 0 else z - 1
        return pltpu.make_async_remote_copy(tok.at[b], tok.at[b], tsend.at[dirn, k], trecv.at[dirn, k],
                                            device_id={"tp": dev}, device_id_type=MESH)

    def has_out(dirn, k):
        return (z - k >= 0) & not_last if dirn == 0 else (z + k <= T - 1) & not_first

    def has_in(dirn, k):
        return z - k - 1 >= 0 if dirn == 0 else z + k + 1 <= T - 1

    def tok_step(k):
        for dirn in range(2):
            if k > 0:
                @pl.when(has_in(dirn, k - 1))
                def _():
                    tok_in(dirn, k - 1).wait_recv()
            if k < T - 1:
                @pl.when(has_out(dirn, k))
                def _():
                    tok_out(dirn, k).start()

    tok_step(0)

    for m in range(2):
        loads(m, 0).wait()
        for q in range(NC):
            convert(m, pl.multiple_of(g * piece, piece) + q * CR, CR)
            for d in range(1, Y):
                y_copy(m, d, q).start()
        for e in range(1, G):
            loads(m, e).wait()
            convert(m, pl.multiple_of(((g + e) % G) * piece, piece), piece)
        own_copy(m, True).start()

    def fwd(m, q):
        for d in range(1, Y):
            if q < NC:
                y_in(m, d, q).wait_recv()
                for e in range(1, G):
                    x_copy(m, d, q, e).start()
                c_copy(m, d, q, 0).start()
            if q >= LAG:
                for e in range(1, G):
                    x_in(m, d, q - LAG, e).wait_recv()
                    c_copy(m, d, q - LAG, e).start()

    LAG = 2
    steps = NC + LAG
    tok_at = {max(1, (steps * k) // (T - 1)): k for k in range(1, T - 1)}
    for q in range(steps):
        fwd(0, q)
        if q in tok_at:
            tok_step(tok_at[q])
    for k in range(1, T - 1):
        if k not in tok_at.values():
            tok_step(k)
    own_copy(0, False).wait_recv()
    for d in range(1, Y):
        for q in range(NC):
            for e in range(G):
                c_in(0, d, q, e).wait_recv()

    NT = min(512, H)

    def first_mm(t):
        x = tok[t]
        @pl.loop(0, H // NT)
        def _(j):
            cols = pl.ds(pl.multiple_of(j * NT, NT), NT)
            l = jnp.maximum(jnp.dot(x, up_full[:, cols], preferred_element_type=F32), 0.0)
            hidden[t, :, cols] = (l * l).astype(BF16)

    def second_mm(t, f):
        w = down_full[pl.ds(pl.multiple_of(f * R, R), R), :]
        return lax.dot_general(hidden[t], w, (((1,), (1,)), ((), ())), preferred_element_type=F32).astype(BF16)

    side = jnp.minimum(z, T - 1 - z)

    def order(k):
        n = T - 1 - k
        near = jnp.where(n % 2 == 1, z + (n + 1) // 2, z - n // 2)
        far = jnp.where(z < T - 1 - z, z + (n - side), z - (n - side))
        return jnp.where(n <= 2 * side, near, far)

    def rs_copy(t, f, right):
        dev = z + 1 if right else z - 1
        slot = t if right else jnp.where(t == z - 1, T, t)
        return pltpu.make_async_remote_copy(sbuf.at[t, f], rbuf.at[slot, f], rsend.at[t, f], rrecv.at[slot, f],
                                            device_id={"tp": dev}, device_id_type=MESH)

    def rs_in(slot, f):
        return pltpu.make_async_remote_copy(sbuf.at[0, f], rbuf.at[slot, f], rsend.at[0, f], rrecv.at[slot, f],
                                            device_id={"tp": z}, device_id_type=MESH)

    def unit(t, f):
        p = second_mm(t, f)
        inner = ((t > z) & not_first) | ((t < z) & not_last)

        @pl.when(inner)
        def _():
            rs_in(t, f).wait_recv()
            sbuf[t, f] = (p.astype(F32) + rbuf[t, f].astype(F32)).astype(BF16)

        @pl.when(jnp.logical_not(inner))
        def _():
            sbuf[t, f] = p

        @pl.when(t > z)
        def _():
            rs_copy(t, f, True).start()

        @pl.when(t < z)
        def _():
            rs_copy(t, f, False).start()

    def feature(d, other):
        return ((y - d + Y) % Y) * 2 + (1 - c if other else c)

    def own_unit(f):
        cols = pl.ds(pl.multiple_of(f * R, R), R)
        total[:, cols] = second_mm(z, f).astype(F32)

    own_copy(1, False).wait_recv()
    todo = list(range(steps))

    def some(n):
        for _ in range(n):
            if todo:
                fwd(1, todo.pop(0))

    for k in range(T):
        t = order(k) if k < T - 1 else z
        if k == 0:
            tok_step(T - 1)
        first_mm(t)
        some(1)
        for other in range(2):
            if k < T - 1:
                unit(t, feature(0, other))
            else:
                own_unit(feature(0, other))
            some(1)
    some(len(todo))
    for d in range(1, Y):
        for q in range(NC):
            for e in range(G):
                c_in(1, d, q, e).wait_recv()
    for d in range(1, Y):
        for other in range(2):
            f = feature(d, other)
            for k in range(T - 1):
                unit(order(k), f)
            own_unit(f)

    for f in range(F):
        cols = pl.ds(f * R, R)

        @pl.when(not_first)
        def _():
            rs_in(z, f).wait_recv()
            total[:, cols] += rbuf[z, f].astype(F32)

        @pl.when(not_last)
        def _():
            rs_in(T, f).wait_recv()
            total[:, cols] += rbuf[T, f].astype(F32)

    s = total[...]
    inv = lax.rsqrt(jnp.mean(s * s, axis=1, keepdims=True) + 1e-06)
    mixed_ref[...] = (s * inv * post_ref[...]).astype(BF16)

    for k in range(T - 1):
        for dirn in range(2):
            @pl.when(has_out(dirn, k))
            def _():
                tok_out(dirn, k).wait_send()
    for m in range(2):
        own_copy(m, True).wait_send()
        for d in range(1, Y):
            for q in range(NC):
                y_copy(m, d, q).wait_send()
                for e in range(G):
                    if e:
                        x_copy(m, d, q, e).wait_send()
                    c_copy(m, d, q, e).wait_send()
    for k in range(T - 1):
        t = order(k)
        for f in range(F):
            rs_copy(t, f, True).wait_send()


def out_kernel(up_v, down_v, up_o, down_o, sem):
    n = sem.shape[1]
    r = up_v.shape[0] // n
    cps = [pltpu.make_async_copy(a.at[pl.ds(i * r, r)], b.at[pl.ds(i * r, r)], sem.at[m, i])
           for m, (a, b) in enumerate(((up_v, up_o), (down_v, down_o))) for i in range(n)]
    for cp in cps:
        cp.start()
    for cp in cps:
        cp.wait()


def solution(mesh):
    G, F, T = mesh.shape["grp"], mesh.shape["fs"], mesh.shape["tp"]
    Y = F // 2

    def per_device(prompt_tokens, up_weight, down_weight, pre_gain, post_gain):
        rows, D = prompt_tokens.shape
        R, H = up_weight.shape
        piece = R // G
        CR = max(16, piece // 8)
        NC = piece // CR
        DMA = pltpu.SemaphoreType.DMA
        vm, any_ = pl.BlockSpec(memory_space=pltpu.VMEM), pl.BlockSpec(memory_space=pl.ANY)
        mixed, up, down = pl.pallas_call(
            functools.partial(layer_kernel, (G, F, T, NC)),
            out_shape=(jax.ShapeDtypeStruct((rows, D), BF16),
                       pltpu.VMEM((F * R, H), BF16), pltpu.VMEM((F * R, H), BF16)),
            in_specs=[vm, vm, vm, any_, any_],
            out_specs=(vm, vm, vm),
            scratch_shapes=[
                pltpu.VMEM((2, R, H), F32),
                pltpu.VMEM((T, rows, D), BF16),
                pltpu.VMEM((T, rows, H), BF16),
                pltpu.VMEM((T + 1, F, rows, R), BF16),
                pltpu.VMEM((T, F, rows, R), BF16),
                pltpu.VMEM((rows, D), F32),
                DMA((2, G)), DMA((2, T)), DMA((2, T)),
                DMA((2, Y, NC)), DMA((2, Y, NC)),
                DMA((2, Y, NC, G)), DMA((2, Y, NC, G)),
                DMA((2, Y, NC, G)), DMA((2, Y, NC, G)),
                DMA((2,)), DMA((2,)),
                DMA((T, F)), DMA((T + 1, F)),
            ],
            compiler_params=pltpu.CompilerParams(collective_id=0, has_side_effects=True,
                                                 vmem_limit_bytes=40 * 1024 * 1024),
            name="layer",
        )(prompt_tokens, pre_gain.reshape(R, 1), post_gain.reshape(1, D), up_weight, down_weight)
        whole = jax.ShapeDtypeStruct((F * R, H), BF16)
        up_o, down_o = pl.pallas_call(
            out_kernel, out_shape=(whole, whole), in_specs=[vm, vm], out_specs=(any_, any_),
            scratch_shapes=[DMA((2, 8))], name="put",
        )(up, down)
        return mixed, up_o, down_o

    placed = (P(("grp", "fs", "tp"), None), P("fs", "tp"), P("fs", "tp"), P("fs"), P())
    return jax.shard_map(
        per_device,
        mesh=mesh,
        in_specs=placed,
        out_specs=(P(("grp", "fs", "tp"), None), P("grp", "tp"), P("grp", "tp")),
        check_vma=False,
    )
```

```python
import functools

import jax
import jax.numpy as jnp
from jax import lax
from jax.experimental import pallas as pl
from jax.experimental.pallas import tpu as pltpu
from jax.sharding import PartitionSpec as P

MESH = pl.DeviceIdType.MESH
S = 2
BF16 = jnp.bfloat16
F32 = jnp.float32


def layer_kernel(sizes, tok_ref, gain_ref, post_ref, up_hbm, down_hbm, mixed_ref, up_full, down_full,
                 stage, gain_cols, tok, hidden, rbuf, sbuf, total,
                 first_sem, load_sem, tsend, trecv, ysend, yrecv, xsend, xrecv, csend, crecv, osend, orecv, rsend, rrecv):
    G, F, T, NC = sizes
    Y = F // 2
    g, fs, z = lax.axis_index("grp"), lax.axis_index("fs"), lax.axis_index("tp")
    y, c = fs // 2, fs % 2
    R, H = up_hbm.shape
    piece = R // G
    CR = piece // NC
    rows_t = tok_ref.shape[0]
    full = (up_full, down_full)
    hbm = (up_hbm, down_hbm)
    partner = y * 2 + (1 - c)
    not_first, not_last = z > 0, z < T - 1

    def loads(m, e):
        r = pl.ds(pl.multiple_of(((g + e) % G) * piece, piece), piece)
        return pltpu.make_async_copy(hbm[m].at[r], stage.at[m, r], load_sem.at[m, e])

    def first_load(q):
        r = pl.ds(pl.multiple_of(g * piece + q * CR, CR), CR)
        return pltpu.make_async_copy(up_hbm.at[r], stage.at[0, r], first_sem.at[q])

    for q in range(NC):
        first_load(q).start()
    for m, e in [(1, 0)] + [(m, e) for m in range(2) for e in range(1, G)]:
        loads(m, e).start()

    barrier = pltpu.get_barrier_semaphore()
    for d in range(1, Y):
        pl.semaphore_signal(barrier, inc=1, device_id={"fs": ((y + d) % Y) * 2 + c}, device_id_type=MESH)
    for e in range(1, G):
        pl.semaphore_signal(barrier, inc=1, device_id={"grp": (g + e) % G}, device_id_type=MESH)
    pl.semaphore_signal(barrier, inc=1, device_id={"fs": partner}, device_id_type=MESH)

    @pl.when(not_first)
    def _():
        pl.semaphore_signal(barrier, inc=1, device_id={"tp": z - 1}, device_id_type=MESH)

    @pl.when(not_last)
    def _():
        pl.semaphore_signal(barrier, inc=1, device_id={"tp": z + 1}, device_id_type=MESH)

    L = gain_cols.shape[1]
    for i in range(0, R, L):
        gain_cols[i:i + L, :] = jnp.transpose(jnp.broadcast_to(gain_ref[:, i:i + L], (L, L)))

    values = tok_ref[...].astype(F32)
    scale = lax.rsqrt(jnp.mean(values * values, axis=1, keepdims=True) + 1e-06)
    tok[z] = (values * scale).astype(BF16)

    def convert(m, start, n):
        for i in range(0, n, CR):
            r = pl.ds(pl.multiple_of(start + i, CR), CR)
            v = stage[m, r, :]
            if m == 0:
                v = v * gain_cols[r, 0:1]
            full[m][pl.ds(pl.multiple_of(fs * R + start + i, CR), CR), :] = v.astype(BF16)

    def remote(ref, rows, ss, rs, dev):
        return pltpu.make_async_remote_copy(ref.at[rows], ref.at[rows], ss, rs, device_id=dev, device_id_type=MESH)

    def chunk_rows(shard, e, q):
        return pl.ds(pl.multiple_of(shard * R + ((g + e) % G) * piece + q * CR, CR), CR)

    def y_copy(m, d, q):
        return remote(full[m], chunk_rows(fs, 0, q), ysend.at[m, d, q], yrecv.at[m, d, q],
                      {"fs": ((y + d) % Y) * 2 + c})

    def y_in(m, d, q):
        shard = ((y - d + Y) % Y) * 2 + c
        return remote(full[m], chunk_rows(shard, 0, q), ysend.at[m, d, q], yrecv.at[m, d, q], {"fs": partner})

    def x_copy(m, d, q, e):
        shard = ((y - d + Y) % Y) * 2 + c
        return remote(full[m], chunk_rows(shard, 0, q), xsend.at[m, d, q, e], xrecv.at[m, d, q, e],
                      {"grp": (g + e) % G})

    def x_in(m, d, q, e):
        shard = ((y - d + Y) % Y) * 2 + c
        return remote(full[m], chunk_rows(shard, G - e, q), xsend.at[m, d, q, e], xrecv.at[m, d, q, e],
                      {"grp": (g + e) % G})

    def c_copy(m, d, q, e):
        shard = ((y - d + Y) % Y) * 2 + c
        return remote(full[m], chunk_rows(shard, (G - e) % G, q), csend.at[m, d, q, e], crecv.at[m, d, q, e],
                      {"fs": partner})

    def c_in(m, d, q, e):
        shard = ((y - d + Y) % Y) * 2 + (1 - c)
        return remote(full[m], chunk_rows(shard, (G - e) % G, q), csend.at[m, d, q, e], crecv.at[m, d, q, e],
                      {"fs": partner})

    def own_copy(m, sign):
        shard = fs if sign else partner
        r = pl.ds(pl.multiple_of(shard * R, R), R)
        return remote(full[m], r, osend.at[m], orecv.at[m], {"fs": partner})

    pl.semaphore_wait(barrier, (Y - 1) + (G - 1) + 1 + not_first.astype(jnp.int32) + not_last.astype(jnp.int32))

    def tok_move(dirn, k, p, b):
        dev = z + 1 if dirn == 0 else z - 1
        r = pl.ds(p * (rows_t // S), rows_t // S)
        return pltpu.make_async_remote_copy(tok.at[b, r], tok.at[b, r], tsend.at[dirn, k, p], trecv.at[dirn, k, p],
                                            device_id={"tp": dev}, device_id_type=MESH)

    def tok_out(dirn, k, p):
        return tok_move(dirn, k, p, z - k if dirn == 0 else z + k)

    def tok_in(dirn, k, p):
        return tok_move(dirn, k, p, z - k - 1 if dirn == 0 else z + k + 1)

    def has_out(dirn, k):
        return (z - k >= 0) & not_last if dirn == 0 else (z + k <= T - 1) & not_first

    def has_in(dirn, k):
        return z - k - 1 >= 0 if dirn == 0 else z + k + 1 <= T - 1

    def tok_step(k, p):
        for dirn in range(2):
            if k > 0:
                @pl.when(has_in(dirn, k - 1))
                def _():
                    tok_in(dirn, k - 1, p).wait_recv()
            if k < T - 1:
                @pl.when(has_out(dirn, k))
                def _():
                    tok_out(dirn, k, p).start()

    for p in range(S):
        tok_step(0, p)

    for m in range(2):
        if m:
            loads(m, 0).wait()
        for q in range(NC):
            if not m:
                first_load(q).wait()
            convert(m, pl.multiple_of(g * piece, piece) + q * CR, CR)
            for d in range(1, Y):
                y_copy(m, d, q).start()
        for e in range(1, G):
            loads(m, e).wait()
            convert(m, pl.multiple_of(((g + e) % G) * piece, piece), piece)
        own_copy(m, True).start()

    def fwd(m, q):
        for d in range(1, Y):
            if q < NC:
                y_in(m, d, q).wait_recv()
                for e in range(1, G):
                    x_copy(m, d, q, e).start()
                c_copy(m, d, q, 0).start()
            if q >= LAG:
                for e in range(1, G):
                    x_in(m, d, q - LAG, e).wait_recv()
                    c_copy(m, d, q - LAG, e).start()

    LAG = 2
    steps = NC + LAG
    tok_steps = [(k, p) for k in range(1, T - 1) for p in range(S)]
    for q in range(steps):
        fwd(0, q)
        if q % 2 == 1 and tok_steps:
            tok_step(*tok_steps.pop(0))
    for k, p in tok_steps:
        tok_step(k, p)
    own_copy(0, False).wait_recv()
    for d in range(1, Y):
        for q in range(NC):
            for e in range(G):
                c_in(0, d, q, e).wait_recv()

    NT = min(512, H)

    def first_mm(t):
        x = tok[t]
        @pl.loop(0, H // NT)
        def _(j):
            cols = pl.ds(pl.multiple_of(j * NT, NT), NT)
            l = jnp.maximum(jnp.dot(x, up_full[:, cols], preferred_element_type=F32), 0.0)
            hidden[t, :, cols] = (l * l).astype(BF16)

    def second_mm(t, f):
        w = down_full[pl.ds(pl.multiple_of(f * R, R), R), :]
        return lax.dot_general(hidden[t], w, (((1,), (1,)), ((), ())), preferred_element_type=F32).astype(BF16)

    lower = 2 * z < T

    def near(k):
        up = jnp.where(k < T - 1 - z, z + 1 + k, T - 2 - k)
        down = jnp.where(k < z, z - 1 - k, k + 1)
        return jnp.where(lower, up, down)

    def far(k):
        up = jnp.where(k < T - 1 - z, T - 1 - k, k - (T - 1 - z))
        down = jnp.where(k < z, k, T - 1 - (k - z))
        return jnp.where(lower, up, down)

    def rs_copy(t, f, right):
        dev = z + 1 if right else z - 1
        slot = t if right else jnp.where(t == z - 1, T, t)
        return pltpu.make_async_remote_copy(sbuf.at[t, f], rbuf.at[slot, f], rsend.at[t, f], rrecv.at[slot, f],
                                            device_id={"tp": dev}, device_id_type=MESH)

    def rs_in(slot, f):
        return pltpu.make_async_remote_copy(sbuf.at[0, f], rbuf.at[slot, f], rsend.at[0, f], rrecv.at[slot, f],
                                            device_id={"tp": z}, device_id_type=MESH)

    def is_inner(t):
        return ((t > z) & not_first) | ((t < z) & not_last)

    def rs_start(t, f):
        @pl.when(t > z)
        def _():
            rs_copy(t, f, True).start()

        @pl.when(t < z)
        def _():
            rs_copy(t, f, False).start()

    def unit(t, f):
        sbuf[t, f] = second_mm(t, f)

        @pl.when(jnp.logical_not(is_inner(t)))
        def _():
            rs_start(t, f)

    def merge(t, f):
        @pl.when(is_inner(t))
        def _():
            rs_in(t, f).wait_recv()
            sbuf[t, f] = (sbuf[t, f].astype(F32) + rbuf[t, f].astype(F32)).astype(BF16)
            rs_start(t, f)

    def feature(d, other):
        return ((y - d + Y) % Y) * 2 + (1 - c if other else c)

    def own_unit(f):
        cols = pl.ds(pl.multiple_of(f * R, R), R)
        total[:, cols] = second_mm(z, f).astype(F32)

    own_copy(1, False).wait_recv()
    todo = list(range(steps))

    def some(n):
        for _ in range(n):
            if todo:
                fwd(1, todo.pop(0))

    for k in range(T):
        t = near(k) if k < T - 1 else z
        if k == T - 2:
            for p in range(S):
                tok_step(T - 1, p)
        first_mm(t)
        for other in range(2):
            if k < T - 1:
                unit(t, feature(0, other))
                some(1)
            else:
                own_unit(feature(0, other))
    for k in range(T - 1):
        for other in range(2):
            merge(near(k), feature(0, other))
            some(1)
    some(len(todo))
    for d in range(1, Y):
        for q in range(NC):
            for e in range(G):
                c_in(1, d, q, e).wait_recv()
    rest = [feature(d, other) for d in range(1, Y) for other in range(2)]
    for k in range(T - 1):
        for f in rest:
            unit(far(k), f)
    for f in rest:
        own_unit(f)
    for k in range(T - 1):
        for f in rest:
            merge(far(k), f)

    for f in range(F):
        cols = pl.ds(f * R, R)

        @pl.when(not_first)
        def _():
            rs_in(z, f).wait_recv()
            total[:, cols] += rbuf[z, f].astype(F32)

        @pl.when(not_last)
        def _():
            rs_in(T, f).wait_recv()
            total[:, cols] += rbuf[T, f].astype(F32)

    s = total[...]
    inv = lax.rsqrt(jnp.mean(s * s, axis=1, keepdims=True) + 1e-06)
    mixed_ref[...] = (s * inv * post_ref[...]).astype(BF16)

    for k in range(T - 1):
        for dirn in range(2):
            @pl.when(has_out(dirn, k))
            def _():
                [tok_out(dirn, k, p).wait_send() for p in range(S)]
    for m in range(2):
        own_copy(m, True).wait_send()
        for d in range(1, Y):
            for q in range(NC):
                y_copy(m, d, q).wait_send()
                for e in range(G):
                    if e:
                        x_copy(m, d, q, e).wait_send()
                    c_copy(m, d, q, e).wait_send()
    for k in range(T - 1):
        t = near(k)
        for f in range(F):
            rs_copy(t, f, True).wait_send()


def solution(mesh):
    G, F, T = mesh.shape["grp"], mesh.shape["fs"], mesh.shape["tp"]
    Y = F // 2

    def per_device(prompt_tokens, up_weight, down_weight, pre_gain, post_gain):
        rows, D = prompt_tokens.shape
        R, H = up_weight.shape
        piece = R // G
        CR = max(16, piece // 8)
        NC = piece // CR
        L = min(128, R)
        DMA = pltpu.SemaphoreType.DMA
        vm, any_ = pl.BlockSpec(memory_space=pltpu.VMEM), pl.BlockSpec(memory_space=pl.ANY)
        mixed, up, down = pl.pallas_call(
            functools.partial(layer_kernel, (G, F, T, NC)),
            out_shape=(jax.ShapeDtypeStruct((rows, D), BF16),
                       pltpu.VMEM((F * R, H), BF16), pltpu.VMEM((F * R, H), BF16)),
            in_specs=[vm, vm, vm, any_, any_],
            out_specs=(vm, vm, vm),
            scratch_shapes=[
                pltpu.VMEM((2, R, H), F32),
                pltpu.VMEM((R, L), F32),
                pltpu.VMEM((T, rows, D), BF16),
                pltpu.VMEM((T, rows, H), BF16),
                pltpu.VMEM((T + 1, F, rows, R), BF16),
                pltpu.VMEM((T, F, rows, R), BF16),
                pltpu.VMEM((rows, D), F32),
                DMA((NC,)), DMA((2, G)), DMA((2, T, S)), DMA((2, T, S)),
                DMA((2, Y, NC)), DMA((2, Y, NC)),
                DMA((2, Y, NC, G)), DMA((2, Y, NC, G)),
                DMA((2, Y, NC, G)), DMA((2, Y, NC, G)),
                DMA((2,)), DMA((2,)),
                DMA((T, F)), DMA((T + 1, F)),
            ],
            compiler_params=pltpu.CompilerParams(collective_id=0, has_side_effects=True,
                                                 vmem_limit_bytes=40 * 1024 * 1024),
            name="layer",
        )(prompt_tokens, pre_gain.reshape(1, R), post_gain.reshape(1, D), up_weight, down_weight)
        return mixed, up, down

    placed = (P(("grp", "fs", "tp"), None), P("fs", "tp"), P("fs", "tp"), P("fs"), P())
    return jax.shard_map(
        per_device,
        mesh=mesh,
        in_specs=placed,
        out_specs=(P(("grp", "fs", "tp"), None), P("grp", "tp"), P("grp", "tp")),
        check_vma=False,
    )
```

```python
import functools

import jax
import jax.numpy as jnp
from jax import lax
from jax.experimental import pallas as pl
from jax.experimental.pallas import tpu as pltpu
from jax.sharding import PartitionSpec as P

MESH = pl.DeviceIdType.MESH
S = 2
BF16 = jnp.bfloat16
F32 = jnp.float32


def layer_kernel(sizes, tok_ref, gain_ref, post_ref, up_hbm, down_hbm, mixed_ref, up_full, down_full,
                 stage, gain_cols, tok, hidden, rbuf, sbuf, total,
                 first_sem, load_sem, tsend, trecv, ysend, yrecv, xsend, xrecv, csend, crecv, osend, orecv, rsend, rrecv):
    G, F, T, NC = sizes
    Y = F // 2
    g, fs, z = lax.axis_index("grp"), lax.axis_index("fs"), lax.axis_index("tp")
    y, c = fs // 2, fs % 2
    R, H = up_hbm.shape
    piece = R // G
    CR = piece // NC
    rows_t = tok_ref.shape[0]
    full = (up_full, down_full)
    hbm = (up_hbm, down_hbm)
    partner = y * 2 + (1 - c)
    not_first, not_last = z > 0, z < T - 1

    def loads(m, e):
        r = pl.ds(pl.multiple_of(((g + e) % G) * piece, piece), piece)
        return pltpu.make_async_copy(hbm[m].at[r], stage.at[m, r], load_sem.at[m, e])

    def first_load(q):
        r = pl.ds(pl.multiple_of(g * piece + q * CR, CR), CR)
        return pltpu.make_async_copy(up_hbm.at[r], stage.at[0, r], first_sem.at[q])

    for q in range(NC):
        first_load(q).start()
    for m, e in [(1, 0)] + [(m, e) for m in range(2) for e in range(1, G)]:
        loads(m, e).start()

    barrier = pltpu.get_barrier_semaphore()
    for d in range(1, Y):
        pl.semaphore_signal(barrier, inc=1, device_id={"fs": ((y + d) % Y) * 2 + c}, device_id_type=MESH)
    for e in range(1, G):
        pl.semaphore_signal(barrier, inc=1, device_id={"grp": (g + e) % G}, device_id_type=MESH)
    pl.semaphore_signal(barrier, inc=1, device_id={"fs": partner}, device_id_type=MESH)

    @pl.when(not_first)
    def _():
        pl.semaphore_signal(barrier, inc=1, device_id={"tp": z - 1}, device_id_type=MESH)

    @pl.when(not_last)
    def _():
        pl.semaphore_signal(barrier, inc=1, device_id={"tp": z + 1}, device_id_type=MESH)

    L = gain_cols.shape[1]
    for i in range(0, R, L):
        gain_cols[i:i + L, :] = jnp.transpose(jnp.broadcast_to(gain_ref[:, i:i + L], (L, L)))

    values = tok_ref[...].astype(F32)
    scale = lax.rsqrt(jnp.mean(values * values, axis=1, keepdims=True) + 1e-06)
    tok[z] = (values * scale).astype(BF16)

    def convert(m, start, n):
        for i in range(0, n, CR):
            r = pl.ds(pl.multiple_of(start + i, CR), CR)
            v = stage[m, r, :]
            if m == 0:
                v = v * gain_cols[r, 0:1]
            full[m][pl.ds(pl.multiple_of(fs * R + start + i, CR), CR), :] = v.astype(BF16)

    def remote(ref, rows, ss, rs, dev):
        return pltpu.make_async_remote_copy(ref.at[rows], ref.at[rows], ss, rs, device_id=dev, device_id_type=MESH)

    def chunk_rows(shard, e, q):
        return pl.ds(pl.multiple_of(shard * R + ((g + e) % G) * piece + q * CR, CR), CR)

    def y_copy(m, d, q):
        return remote(full[m], chunk_rows(fs, 0, q), ysend.at[m, d, q], yrecv.at[m, d, q],
                      {"fs": ((y + d) % Y) * 2 + c})

    def y_in(m, d, q):
        shard = ((y - d + Y) % Y) * 2 + c
        return remote(full[m], chunk_rows(shard, 0, q), ysend.at[m, d, q], yrecv.at[m, d, q], {"fs": partner})

    def x_copy(m, d, q, e):
        shard = ((y - d + Y) % Y) * 2 + c
        return remote(full[m], chunk_rows(shard, 0, q), xsend.at[m, d, q, e], xrecv.at[m, d, q, e],
                      {"grp": (g + e) % G})

    def x_in(m, d, q, e):
        shard = ((y - d + Y) % Y) * 2 + c
        return remote(full[m], chunk_rows(shard, G - e, q), xsend.at[m, d, q, e], xrecv.at[m, d, q, e],
                      {"grp": (g + e) % G})

    def c_copy(m, d, q, e):
        shard = ((y - d + Y) % Y) * 2 + c
        return remote(full[m], chunk_rows(shard, (G - e) % G, q), csend.at[m, d, q, e], crecv.at[m, d, q, e],
                      {"fs": partner})

    def c_in(m, d, q, e):
        shard = ((y - d + Y) % Y) * 2 + (1 - c)
        return remote(full[m], chunk_rows(shard, (G - e) % G, q), csend.at[m, d, q, e], crecv.at[m, d, q, e],
                      {"fs": partner})

    def own_copy(m, sign):
        shard = fs if sign else partner
        r = pl.ds(pl.multiple_of(shard * R, R), R)
        return remote(full[m], r, osend.at[m], orecv.at[m], {"fs": partner})

    pl.semaphore_wait(barrier, (Y - 1) + (G - 1) + 1 + not_first.astype(jnp.int32) + not_last.astype(jnp.int32))

    def tok_move(dirn, k, p, b):
        dev = z + 1 if dirn == 0 else z - 1
        r = pl.ds(p * (rows_t // S), rows_t // S)
        return pltpu.make_async_remote_copy(tok.at[b, r], tok.at[b, r], tsend.at[dirn, k, p], trecv.at[dirn, k, p],
                                            device_id={"tp": dev}, device_id_type=MESH)

    def tok_out(dirn, k, p):
        return tok_move(dirn, k, p, z - k if dirn == 0 else z + k)

    def tok_in(dirn, k, p):
        return tok_move(dirn, k, p, z - k - 1 if dirn == 0 else z + k + 1)

    def has_out(dirn, k):
        return (z - k >= 0) & not_last if dirn == 0 else (z + k <= T - 1) & not_first

    def has_in(dirn, k):
        return z - k - 1 >= 0 if dirn == 0 else z + k + 1 <= T - 1

    def tok_step(k, p):
        for dirn in range(2):
            if k > 0:
                @pl.when(has_in(dirn, k - 1))
                def _():
                    tok_in(dirn, k - 1, p).wait_recv()
            if k < T - 1:
                @pl.when(has_out(dirn, k))
                def _():
                    tok_out(dirn, k, p).start()

    for p in range(S):
        tok_step(0, p)

    for m in range(2):
        if m:
            loads(m, 0).wait()
        for q in range(NC):
            if not m:
                first_load(q).wait()
            convert(m, pl.multiple_of(g * piece, piece) + q * CR, CR)
            for d in range(1, Y):
                y_copy(m, d, q).start()
        for e in range(1, G):
            loads(m, e).wait()
            convert(m, pl.multiple_of(((g + e) % G) * piece, piece), piece)
        own_copy(m, True).start()

    def fwd(m, q):
        for d in range(1, Y):
            if q < NC:
                y_in(m, d, q).wait_recv()
                for e in range(1, G):
                    x_copy(m, d, q, e).start()
                c_copy(m, d, q, 0).start()
            if q >= LAG:
                for e in range(1, G):
                    x_in(m, d, q - LAG, e).wait_recv()
                    c_copy(m, d, q - LAG, e).start()

    LAG = 2
    steps = NC + LAG
    TOK_GAP = max(2, NC // 4)
    tok_steps = [(k, p) for k in range(1, T - 1) for p in range(S)]
    for q in range(steps):
        fwd(0, q)
        if q % TOK_GAP == TOK_GAP - 1 and tok_steps:
            tok_step(*tok_steps.pop(0))
    for k, p in tok_steps:
        tok_step(k, p)
    own_copy(0, False).wait_recv()
    for d in range(1, Y):
        for q in range(NC):
            for e in range(G):
                c_in(0, d, q, e).wait_recv()

    NT = min(512, H)

    def first_mm(t):
        x = tok[t]
        @pl.loop(0, H // NT)
        def _(j):
            cols = pl.ds(pl.multiple_of(j * NT, NT), NT)
            l = jnp.maximum(jnp.dot(x, up_full[:, cols], preferred_element_type=F32), 0.0)
            hidden[t, :, cols] = (l * l).astype(BF16)

    def second_mm(t, f):
        w = down_full[pl.ds(pl.multiple_of(f * R, R), R), :]
        return lax.dot_general(hidden[t], w, (((1,), (1,)), ((), ())), preferred_element_type=F32).astype(BF16)

    lower = 2 * z < T

    def near(k):
        up = jnp.where(k < T - 1 - z, z + 1 + k, T - 2 - k)
        down = jnp.where(k < z, z - 1 - k, k + 1)
        return jnp.where(lower, up, down)

    def far(k):
        up = jnp.where(k < T - 1 - z, T - 1 - k, k - (T - 1 - z))
        down = jnp.where(k < z, k, T - 1 - (k - z))
        return jnp.where(lower, up, down)

    def rs_copy(t, f, right):
        dev = z + 1 if right else z - 1
        slot = t if right else jnp.where(t == z - 1, T, t)
        return pltpu.make_async_remote_copy(sbuf.at[t, f], rbuf.at[slot, f], rsend.at[t, f], rrecv.at[slot, f],
                                            device_id={"tp": dev}, device_id_type=MESH)

    def rs_in(slot, f):
        return pltpu.make_async_remote_copy(sbuf.at[0, f], rbuf.at[slot, f], rsend.at[0, f], rrecv.at[slot, f],
                                            device_id={"tp": z}, device_id_type=MESH)

    def is_inner(t):
        return ((t > z) & not_first) | ((t < z) & not_last)

    def rs_start(t, f):
        @pl.when(t > z)
        def _():
            rs_copy(t, f, True).start()

        @pl.when(t < z)
        def _():
            rs_copy(t, f, False).start()

    def unit(t, f):
        sbuf[t, f] = second_mm(t, f)

        @pl.when(jnp.logical_not(is_inner(t)))
        def _():
            rs_start(t, f)

    def merge(t, f):
        @pl.when(is_inner(t))
        def _():
            rs_in(t, f).wait_recv()
            sbuf[t, f] = (sbuf[t, f].astype(F32) + rbuf[t, f].astype(F32)).astype(BF16)
            rs_start(t, f)

    def feature(d, other):
        return ((y - d + Y) % Y) * 2 + (1 - c if other else c)

    def own_unit(f):
        cols = pl.ds(pl.multiple_of(f * R, R), R)
        total[:, cols] = second_mm(z, f).astype(F32)

    own_copy(1, False).wait_recv()
    todo = list(range(steps))

    def some(n):
        for _ in range(n):
            if todo:
                fwd(1, todo.pop(0))

    for k in range(T):
        t = near(k) if k < T - 1 else z
        if k == T - 2:
            for p in range(S):
                tok_step(T - 1, p)
        first_mm(t)
        for other in range(2):
            if k < T - 1:
                unit(t, feature(0, other))
                some(-(-steps // 12))
            else:
                own_unit(feature(0, other))
    for k in range(T - 1):
        for other in range(2):
            merge(near(k), feature(0, other))
            some(-(-steps // 12))
    some(len(todo))
    for d in range(1, Y):
        for q in range(NC):
            for e in range(G):
                c_in(1, d, q, e).wait_recv()
    rest = [feature(d, other) for d in range(1, Y) for other in range(2)]
    for k in range(T - 1):
        for f in rest:
            unit(far(k), f)
    for f in rest:
        own_unit(f)
    for k in range(T - 1):
        for f in rest:
            merge(far(k), f)

    for f in range(F):
        cols = pl.ds(f * R, R)

        @pl.when(not_first)
        def _():
            rs_in(z, f).wait_recv()
            total[:, cols] += rbuf[z, f].astype(F32)

        @pl.when(not_last)
        def _():
            rs_in(T, f).wait_recv()
            total[:, cols] += rbuf[T, f].astype(F32)

    s = total[...]
    inv = lax.rsqrt(jnp.mean(s * s, axis=1, keepdims=True) + 1e-06)
    mixed_ref[...] = (s * inv * post_ref[...]).astype(BF16)

    for k in range(T - 1):
        for dirn in range(2):
            @pl.when(has_out(dirn, k))
            def _():
                [tok_out(dirn, k, p).wait_send() for p in range(S)]
    for m in range(2):
        own_copy(m, True).wait_send()
        for d in range(1, Y):
            for q in range(NC):
                y_copy(m, d, q).wait_send()
                for e in range(G):
                    if e:
                        x_copy(m, d, q, e).wait_send()
                    c_copy(m, d, q, e).wait_send()
    for k in range(T - 1):
        t = near(k)
        for f in range(F):
            rs_copy(t, f, True).wait_send()


def solution(mesh):
    G, F, T = mesh.shape["grp"], mesh.shape["fs"], mesh.shape["tp"]
    Y = F // 2

    def per_device(prompt_tokens, up_weight, down_weight, pre_gain, post_gain):
        rows, D = prompt_tokens.shape
        R, H = up_weight.shape
        piece = R // G
        CR = max(16, piece // 16)
        NC = piece // CR
        L = min(128, R)
        DMA = pltpu.SemaphoreType.DMA
        vm, any_ = pl.BlockSpec(memory_space=pltpu.VMEM), pl.BlockSpec(memory_space=pl.ANY)
        mixed, up, down = pl.pallas_call(
            functools.partial(layer_kernel, (G, F, T, NC)),
            out_shape=(jax.ShapeDtypeStruct((rows, D), BF16),
                       pltpu.VMEM((F * R, H), BF16), pltpu.VMEM((F * R, H), BF16)),
            in_specs=[vm, vm, vm, any_, any_],
            out_specs=(vm, vm, vm),
            scratch_shapes=[
                pltpu.VMEM((2, R, H), F32),
                pltpu.VMEM((R, L), F32),
                pltpu.VMEM((T, rows, D), BF16),
                pltpu.VMEM((T, rows, H), BF16),
                pltpu.VMEM((T + 1, F, rows, R), BF16),
                pltpu.VMEM((T, F, rows, R), BF16),
                pltpu.VMEM((rows, D), F32),
                DMA((NC,)), DMA((2, G)), DMA((2, T, S)), DMA((2, T, S)),
                DMA((2, Y, NC)), DMA((2, Y, NC)),
                DMA((2, Y, NC, G)), DMA((2, Y, NC, G)),
                DMA((2, Y, NC, G)), DMA((2, Y, NC, G)),
                DMA((2,)), DMA((2,)),
                DMA((T, F)), DMA((T + 1, F)),
            ],
            compiler_params=pltpu.CompilerParams(collective_id=0, has_side_effects=True,
                                                 vmem_limit_bytes=40 * 1024 * 1024),
            name="layer",
        )(prompt_tokens, pre_gain.reshape(1, R), post_gain.reshape(1, D), up_weight, down_weight)
        return mixed, up, down

    placed = (P(("grp", "fs", "tp"), None), P("fs", "tp"), P("fs", "tp"), P("fs"), P())
    return jax.shard_map(
        per_device,
        mesh=mesh,
        in_specs=placed,
        out_specs=(P(("grp", "fs", "tp"), None), P("grp", "tp"), P("grp", "tp")),
        check_vma=False,
    )
```
